32 devices in a mesh: ep: 8 (over z, core), tp: 4 (over y, x).
Axes of the slice: x: 2, y: 2, z: 4, core: 2. Of those that a mesh axis runs over, the one named last changes fastest.
Arguments:
- tokens: bfloat16 [256, 4096], P('ep'), may hold values from -6 to 6
- recur_state: float32 [256, 4096], P('ep', 'tp'), may hold values from -6 to 6
- conv_state: bfloat16 [256, 3, 4096], P('ep', None, 'tp'), may hold values from -6 to 6
- mix_gain: float32 [4096], replicated, may hold values from 0.1 to 1.9
- in_weight: bfloat16 [4096, 4096], P('ep', 'tp'), may hold values from -0.09375 to 0.09375
- gate_weight: bfloat16 [4096, 4096], P('ep', 'tp'), may hold values from -0.09375 to 0.09375
- conv_taps: float32 [4, 4096], P(None, 'tp'), may hold values from -3 to 3
- recur_gate_blocks: bfloat16 [64, 64, 64], P('tp'), may hold values from -0.75 to 0.75
- input_gate_blocks: bfloat16 [64, 64, 64], P('tp'), may hold values from -0.75 to 0.75
- decay_rate: float32 [4096], P('tp'), may hold values from 0.01 to 0.4
- out_weight: bfloat16 [4096, 4096], P('tp', 'ep'), may hold values from -0.09375 to 0.09375
- ffn_gain: float32 [4096], replicated, may hold values from 0.1 to 1.9
- router_weight: bfloat16 [4096, 8], replicated, may hold values from -0.09375 to 0.09375
- routes: int32 [256, 2], P('ep'), may hold values from 0 to 7, as said below
- expert_gate: bfloat16 [8, 4096, 2048], P('ep', None, 'tp'), may hold values from -0.09375 to 0.09375
- expert_up: bfloat16 [8, 4096, 2048], P('ep', None, 'tp'), may hold values from -0.09375 to 0.09375
- expert_down: bfloat16 [8, 2048, 4096], P('ep', 'tp'), may hold values from -0.125 to 0.125
- dense_gate: bfloat16 [4096, 2048], P('ep', 'tp'), may hold values from -0.09375 to 0.09375
- dense_up: bfloat16 [4096, 2048], P('ep', 'tp'), may hold values from -0.09375 to 0.09375
- dense_down: bfloat16 [2048, 4096], P('tp', 'ep'), may hold values from -0.125 to 0.125
- branch_gate: bfloat16 [4096], replicated, may hold values from -0.09375 to 0.09375
Outputs:
- layer_out: bfloat16 [256, 4096], P('ep')
- new_state: float32 [256, 4096], P('ep', 'tp')
- new_conv_state: bfloat16 [256, 3, 4096], P('ep', None, 'tp')
The draws below stay inside these ranges and needn't reach their ends.
Inputs may be any that keep to these rules, and one draw needn't show every extreme that they name: `routes`: A row names two different experts of one group: both have the same e // 4. In the rows of one index of ep no expert is named more than 16 times, and in every draw some expert is named exactly 16 times by the rows of every index of ep.
All inputs are finite; a program needn't handle non-finite values.
Results may differ from the reference program's by a relative error of at most 0.023.
Values may be sent and summed in bfloat16 or wider, within the bound.
A program may use at most 64 MiB of HBM per device.

```python
import math
import jax
import jax.numpy as jnp
from jax import lax

D = 4096
D_A = 4096
BLOCK = 64
FF = 2048
FFD = 2048
CONV_W = 4
TOP_K = 2
E_PER_GROUP = 4
B_DEV = 32
B = 256
EXPERTS = 8
CAP = 16
H_A = 64
N_EP = 8
N_TP = 4


def draw_routes(key, part):
    group_count = EXPERTS // E_PER_GROUP
    group_tokens = 2 * CAP
    slot_count = group_count * group_tokens
    base_group = jax.random.randint(jax.random.fold_in(key, 11), (), 0, group_count)

    def one_block(block):
        block_key = jax.random.fold_in(key, 1000 + block)
        full_group = (block + base_group) % group_count
        scores = jax.random.randint(jax.random.fold_in(block_key, 1), (slot_count,), 0, 1 << 20)
        slot_index = jnp.arange(slot_count, dtype=jnp.int32)
        keyed = jnp.where(slot_index // group_tokens == full_group, 0, scores + 1) * slot_count + slot_index
        chosen = jnp.argsort(keyed)[:B_DEV]
        chosen = chosen[jax.random.permutation(jax.random.fold_in(block_key, 2), B_DEV)]
        group = chosen // group_tokens
        pair = chosen % group_tokens
        member_scores = jax.random.randint(jax.random.fold_in(block_key, 3), (group_count, E_PER_GROUP), 0, 1 << 20) * E_PER_GROUP + jnp.arange(E_PER_GROUP, dtype=jnp.int32)[None, :]
        members = jnp.argsort(member_scores, axis=1).astype(jnp.int32)
        first = members[group, 2 * pair % E_PER_GROUP]
        second = members[group, (2 * pair + 1) % E_PER_GROUP]
        return jnp.stack([group * E_PER_GROUP + first, group * E_PER_GROUP + second], axis=1).astype(jnp.int32)
    return jax.vmap(one_block)(jnp.arange(N_EP, dtype=jnp.int32)).reshape(N_EP * B_DEV, 2)


def block_levels(stream_key, dims, cuts, low, high):
    loudness = 1.0
    for axis_at, blocks in cuts:
        draws = jax.random.uniform(jax.random.fold_in(jax.random.fold_in(stream_key, 6), axis_at), (blocks,), jnp.float32, low / len(cuts), high / len(cuts))
        loudness = loudness * jnp.repeat(jnp.exp(draws), dims[axis_at] // blocks).reshape((-1,) + (1,) * (len(dims) - 1 - axis_at))
    return loudness


def normal_values(stream_key, shape, width, reach, split=(), held_as=jnp.bfloat16):
    entries = width * jax.random.normal(stream_key, shape, jnp.float32)
    if split:
        entries = entries * block_levels(stream_key, shape, split, -0.22, 0.18)
    return jnp.clip(entries, -reach, reach).astype(held_as)


def setup_inputs(seed: int = 0) -> dict:
    streams_of = jax.random.split(jax.random.key(seed), 22)
    tokens = normal_values(streams_of[0], (B, D), 1.0, 6.0, ((0, 8),))
    recur_state = normal_values(streams_of[1], (B, D_A), 1.0, 6.0, ((0, 8), (1, 4)), jnp.float32)
    conv_state = normal_values(streams_of[2], (B, CONV_W - 1, D_A), 1.0, 6.0, ((0, 8), (2, 4)))
    mix_gain = jnp.clip(1.0 + 0.18 * jax.random.normal(streams_of[3], (D,), jnp.float32), 0.1, 1.9)
    in_weight = normal_values(streams_of[4], (D, D_A), D ** -0.5, 0.09375, ((0, 8), (1, 4)))
    gate_weight = normal_values(streams_of[5], (D, D_A), D ** -0.5, 0.09375, ((0, 8), (1, 4)))
    conv_taps = normal_values(streams_of[6], (CONV_W, D_A), 0.5, 3.0, ((1, 4),), jnp.float32)
    recur_gate_blocks = normal_values(streams_of[7], (H_A, BLOCK, BLOCK), BLOCK ** -0.5, 0.75, ((0, 4),))
    input_gate_blocks = normal_values(streams_of[8], (H_A, BLOCK, BLOCK), BLOCK ** -0.5, 0.75, ((0, 4),))
    decay_rate = jnp.clip(jnp.exp(math.log(0.4) - 3.6888795 * jax.random.uniform(streams_of[9], (D_A,), jnp.float32) ** block_levels(streams_of[9], (D_A,), ((0, 4),), -0.2, 0.2)), 0.01, 0.4)
    out_weight = normal_values(streams_of[10], (D_A, D), D_A ** -0.5, 0.09375, ((0, 4), (1, 8)))
    ffn_gain = jnp.clip(1.0 + 0.18 * jax.random.normal(streams_of[11], (D,), jnp.float32), 0.1, 1.9)
    router_weight = normal_values(streams_of[12], (D, EXPERTS), D ** -0.5, 0.09375)
    routes = draw_routes(jax.random.fold_in(streams_of[21], 71), 0)
    expert_gate = normal_values(streams_of[14], (EXPERTS, D, FF), D ** -0.5, 0.09375, ((0, 8), (2, 4)))
    expert_up = normal_values(streams_of[15], (EXPERTS, D, FF), D ** -0.5, 0.09375, ((0, 8), (2, 4)))
    expert_down = normal_values(streams_of[16], (EXPERTS, FF, D), FF ** -0.5, 0.125, ((0, 8), (1, 4)))
    dense_gate = normal_values(streams_of[17], (D, FFD), D ** -0.5, 0.09375, ((0, 8), (1, 4)))
    dense_up = normal_values(streams_of[18], (D, FFD), D ** -0.5, 0.09375, ((0, 8), (1, 4)))
    dense_down = normal_values(streams_of[19], (FFD, D), FFD ** -0.5, 0.125, ((0, 4), (1, 8)))
    branch_gate = normal_values(streams_of[20], (D,), D ** -0.5, 0.09375)
    return dict(tokens=tokens, recur_state=recur_state, conv_state=conv_state, mix_gain=mix_gain, in_weight=in_weight, gate_weight=gate_weight, conv_taps=conv_taps, recur_gate_blocks=recur_gate_blocks, input_gate_blocks=input_gate_blocks, decay_rate=decay_rate, out_weight=out_weight, ffn_gain=ffn_gain, router_weight=router_weight, routes=routes, expert_gate=expert_gate, expert_up=expert_up, expert_down=expert_down, dense_gate=dense_gate, dense_up=dense_up, dense_down=dense_down, branch_gate=branch_gate)


epsilon = 1e-06
decay_scale = 8.0

def rms_scale(rows, gain):
    values = rows.astype(jnp.float32)
    inverse = lax.rsqrt(lax.optimization_barrier(jnp.mean(values * values, axis=-1, keepdims=True)) + epsilon)
    return (values * inverse * gain.astype(jnp.float32)).astype(jnp.bfloat16)

def grouped_product(left, right, groups):
    rows = left.shape[0]
    inner = left.shape[1] // groups
    parts = jnp.einsum('rtf,tfd->trd', left.astype(jnp.float32).reshape(rows, groups, inner), right.astype(jnp.float32).reshape(groups, inner, right.shape[1]))
    rounded = lax.optimization_barrier(parts.astype(jnp.bfloat16))
    return lax.optimization_barrier(jnp.sum(rounded.astype(jnp.float32), axis=0))

def slot_table(routes):
    pairs = routes.reshape(N_EP, B_DEV * TOP_K)
    expert_ids = jnp.arange(EXPERTS, dtype=jnp.int32)
    onehot = (pairs[:, :, None] == expert_ids[None, None, :]).astype(jnp.int32)
    before = jnp.cumsum(onehot, axis=1) - onehot
    rank = lax.optimization_barrier(jnp.sum(before * onehot, axis=2))
    return (pairs * CAP + rank).reshape(N_EP * B_DEV, TOP_K).astype(jnp.int32)

def reference(tokens, recur_state, conv_state, mix_gain, in_weight, gate_weight, conv_taps, recur_gate_blocks, input_gate_blocks, decay_rate, out_weight, ffn_gain, router_weight, routes, expert_gate, expert_up, expert_down, dense_gate, dense_up, dense_down, branch_gate):
    batch_rows = tokens.shape[0]
    normed = rms_scale(tokens, mix_gain)
    x_branch = jnp.dot(normed, in_weight, preferred_element_type=jnp.float32).astype(jnp.bfloat16)
    gate_branch = jnp.dot(normed, gate_weight, preferred_element_type=jnp.float32).astype(jnp.bfloat16)
    window = jnp.concatenate([conv_state, x_branch[:, None, :]], axis=1)
    conv_out = lax.optimization_barrier(jnp.sum(window.astype(jnp.float32) * conv_taps.astype(jnp.float32)[None], axis=1)).astype(jnp.bfloat16)
    new_conv_state = window[:, 1:, :]
    blocks = conv_out.astype(jnp.float32).reshape(batch_rows, H_A, BLOCK)
    recur_gate = jax.nn.sigmoid(jnp.einsum('bhi,hij->bhj', blocks, recur_gate_blocks.astype(jnp.float32)).reshape(batch_rows, D_A))
    input_gate = jax.nn.sigmoid(jnp.einsum('bhi,hij->bhj', blocks, input_gate_blocks.astype(jnp.float32)).reshape(batch_rows, D_A))
    log_decay = -decay_scale * recur_gate * decay_rate
    new_state = jnp.exp(log_decay) * recur_state + jnp.sqrt(-jnp.expm1(2.0 * log_decay)) * input_gate * conv_out.astype(jnp.float32)
    mixer_rows = (new_state * jax.nn.gelu(gate_branch.astype(jnp.float32))).astype(jnp.bfloat16)
    mixed = grouped_product(mixer_rows, out_weight, N_TP)
    resid = (tokens.astype(jnp.float32) + mixed).astype(jnp.bfloat16)
    normed_ffn = rms_scale(resid, ffn_gain)
    router_logits = jnp.dot(normed_ffn, router_weight, preferred_element_type=jnp.float32)
    picked = jnp.take_along_axis(router_logits, routes, axis=1)
    route_weight = jax.nn.sigmoid(picked - picked[:, ::-1]).astype(jnp.bfloat16)
    slots = slot_table(routes)
    global_token = jnp.arange(batch_rows, dtype=jnp.int32)
    source = global_token // B_DEV
    owner = jnp.full((N_EP, EXPERTS * CAP), -1, jnp.int32)
    owner = owner.at[jnp.repeat(source[:, None], TOP_K, axis=1), slots].set(jnp.repeat(global_token[:, None], TOP_K, axis=1))
    table = owner.reshape(N_EP, EXPERTS, CAP).transpose(1, 0, 2).reshape(EXPERTS, N_EP * CAP)

    def serve(item):
        token_index, gate_matrix, up_matrix, down_matrix = item
        valid = token_index >= 0
        rows = jnp.where(valid[:, None], normed_ffn[jnp.maximum(token_index, 0)], jnp.zeros((), jnp.bfloat16))
        first = jnp.dot(rows, gate_matrix, preferred_element_type=jnp.float32)
        second = jnp.dot(rows, up_matrix, preferred_element_type=jnp.float32)
        act = (jax.nn.silu(first) * second).astype(jnp.bfloat16)
        return grouped_product(act, down_matrix, N_TP).astype(jnp.bfloat16)
    expert_rows = lax.map(serve, (table, expert_gate, expert_up, expert_down))
    flat_rows = expert_rows.reshape(EXPERTS * N_EP * CAP, D)
    flat_index = slots // CAP * (N_EP * CAP) + source[:, None] * CAP + slots % CAP
    chosen = flat_rows[flat_index].astype(jnp.float32)
    moe = lax.optimization_barrier(jnp.sum(route_weight.astype(jnp.float32)[:, :, None] * chosen, axis=1))
    dense_first = jnp.dot(normed_ffn, dense_gate, preferred_element_type=jnp.float32)
    dense_second = jnp.dot(normed_ffn, dense_up, preferred_element_type=jnp.float32)
    dense_act = (jax.nn.silu(dense_first) * dense_second).astype(jnp.bfloat16)
    dense_sum = grouped_product(dense_act, dense_down, N_TP)
    branch_weight = jax.nn.sigmoid(jnp.dot(normed_ffn, branch_gate, preferred_element_type=jnp.float32))
    layer_out = (resid.astype(jnp.float32) + moe + branch_weight[:, None] * dense_sum).astype(jnp.bfloat16)
    return (layer_out, new_state, new_conv_state)
```

```python
import functools

import jax
import jax.numpy as jnp
from jax import lax
from jax.experimental import pallas as pl
from jax.experimental.pallas import tpu as pltpu
from jax.sharding import PartitionSpec as P

TOP_K = 2
LANES = 128
F32 = jnp.float32
BF16 = jnp.bfloat16


epsilon = 1e-06
decay_scale = 8.0


def rms_scale(rows, gain):
    values = rows.astype(jnp.float32)
    inverse = lax.rsqrt(jnp.mean(values * values, axis=-1, keepdims=True) + epsilon)
    return (values * inverse * gain).astype(jnp.bfloat16)


def on_device(
    tokens,
    recur_state,
    conv_state,
    mix_gain,
    in_weight,
    gate_weight,
    conv_taps,
    recur_gate_blocks,
    input_gate_blocks,
    decay_rate,
    out_weight,
    ffn_gain,
    router_weight,
    routes,
    expert_gate,
    expert_up,
    expert_down,
    dense_gate,
    dense_up,
    dense_down,
    branch_gate,
):
    batch_rows, width = tokens.shape
    channels = in_weight.shape[1]
    normed = rms_scale(tokens, mix_gain)
    arrived = lax.all_to_all(normed, "ep", split_axis=1, concat_axis=0, tiled=True)
    joined = jnp.concatenate([in_weight, gate_weight], axis=1)
    summed = lax.psum_scatter(
        jnp.dot(arrived, joined, preferred_element_type=jnp.float32).astype(jnp.bfloat16),
        "ep",
        scatter_dimension=0,
        tiled=True,
    ).astype(jnp.float32)
    x_sum, gate_sum = (summed[:, :channels], summed[:, channels:])
    x_branch = x_sum.astype(jnp.bfloat16)
    gate_branch = gate_sum.astype(jnp.bfloat16)
    window = jnp.concatenate([conv_state, x_branch[:, None, :]], axis=1)
    conv_out = jnp.sum(window.astype(jnp.float32) * conv_taps[None], axis=1).astype(jnp.bfloat16)
    new_conv_state = window[:, 1:, :]
    blocks = conv_out.reshape(batch_rows, recur_gate_blocks.shape[0], recur_gate_blocks.shape[1])
    recur_gate = jax.nn.sigmoid(
        jnp.einsum(
            "bhi,hij->bhj", blocks, recur_gate_blocks, preferred_element_type=jnp.float32
        ).reshape(batch_rows, channels)
    )
    input_gate = jax.nn.sigmoid(
        jnp.einsum(
            "bhi,hij->bhj", blocks, input_gate_blocks, preferred_element_type=jnp.float32
        ).reshape(batch_rows, channels)
    )
    log_decay = -decay_scale * recur_gate * decay_rate
    new_state = jnp.exp(log_decay) * recur_state + jnp.sqrt(
        -jnp.expm1(2.0 * log_decay)
    ) * input_gate * conv_out.astype(jnp.float32)
    mixer_rows = (new_state * jax.nn.gelu(gate_branch.astype(jnp.float32))).astype(jnp.bfloat16)
    mixer_part = jnp.dot(
        mixer_rows,
        lax.all_gather(out_weight, "ep", axis=1, tiled=True),
        preferred_element_type=jnp.float32,
    )
    resid = (
        tokens.astype(jnp.float32)
        + lax.psum(mixer_part.astype(jnp.bfloat16), "tp").astype(jnp.float32)
    ).astype(jnp.bfloat16)
    normed_ffn = rms_scale(resid, ffn_gain)
    router_logits = jnp.dot(normed_ffn, router_weight, preferred_element_type=jnp.float32)
    experts = router_logits.shape[1]
    expert_ids = lax.broadcasted_iota(jnp.int32, (batch_rows, TOP_K, experts), 2)
    picked = jnp.sum(
        jnp.where(routes[:, :, None] == expert_ids, router_logits[:, None, :], 0.0), axis=2
    )
    route_weight = jax.nn.sigmoid(picked - picked[:, ::-1]).astype(jnp.bfloat16)
    capacity = 2 * batch_rows * TOP_K // experts
    flat_ids = routes.reshape(batch_rows * TOP_K)
    onehot = (
        flat_ids[:, None] == lax.broadcasted_iota(jnp.int32, (batch_rows * TOP_K, experts), 1)
    ).astype(jnp.int32)
    rank = jnp.sum((jnp.cumsum(onehot, axis=0) - onehot) * onehot, axis=1)
    slot_of = (flat_ids * capacity + rank).reshape(batch_rows, TOP_K)
    slot_rows = lax.broadcasted_iota(jnp.int32, (experts * capacity, batch_rows), 0)
    slot_cols = lax.broadcasted_iota(jnp.int32, (batch_rows, experts * capacity), 1)
    dispatch = jnp.zeros((experts * capacity, batch_rows), jnp.bfloat16)
    combine = jnp.zeros((batch_rows, experts * capacity), jnp.bfloat16)
    for pick in range(TOP_K):
        dispatch = dispatch + (slot_rows == slot_of[None, :, pick]).astype(jnp.bfloat16)
        combine = combine + jnp.where(
            slot_cols == slot_of[:, pick : pick + 1],
            route_weight[:, pick : pick + 1],
            jnp.zeros((), jnp.bfloat16),
        )
    outgoing = (
        jnp.dot(dispatch, normed_ffn, preferred_element_type=jnp.float32)
        .astype(jnp.bfloat16)
        .reshape(experts, capacity, width)
    )
    gate_local = expert_gate[0]
    up_local = expert_up[0]
    down_local = expert_down[0]
    arrived_rows = lax.all_to_all(outgoing, "ep", split_axis=0, concat_axis=0, tiled=True)
    sources, items, features = arrived_rows.shape
    rows = arrived_rows.reshape(sources * items, features)
    first = jnp.dot(rows, gate_local, preferred_element_type=jnp.float32)
    second = jnp.dot(rows, up_local, preferred_element_type=jnp.float32)
    act = (jax.nn.silu(first) * second).astype(jnp.bfloat16)
    partial_value = jnp.dot(act, down_local, preferred_element_type=jnp.float32)
    total = lax.psum(partial_value.astype(jnp.bfloat16), "tp")
    returned = lax.all_to_all(
        total.reshape(sources, items, total.shape[1]), "ep", split_axis=0, concat_axis=0, tiled=True
    )
    moe = jnp.dot(
        combine,
        returned.reshape(experts * capacity, returned.shape[2]),
        preferred_element_type=jnp.float32,
    )
    dense_arrived = lax.all_to_all(normed_ffn, "ep", split_axis=1, concat_axis=0, tiled=True)
    dense_joined = jnp.concatenate([dense_gate, dense_up], axis=1)
    dense_summed = lax.psum_scatter(
        jnp.dot(dense_arrived, dense_joined, preferred_element_type=jnp.float32).astype(
            jnp.bfloat16
        ),
        "ep",
        scatter_dimension=0,
        tiled=True,
    ).astype(jnp.float32)
    dense_first = dense_summed[:, : dense_gate.shape[1]]
    dense_second = dense_summed[:, dense_gate.shape[1] :]
    dense_act = (jax.nn.silu(dense_first) * dense_second).astype(jnp.bfloat16)
    dense_part = jnp.dot(
        dense_act,
        lax.all_gather(dense_down, "ep", axis=1, tiled=True),
        preferred_element_type=jnp.float32,
    )
    branch_weight = jax.nn.sigmoid(
        jnp.dot(normed_ffn, branch_gate, preferred_element_type=jnp.float32)
    )
    dense_sum = lax.psum(dense_part.astype(jnp.bfloat16), "tp").astype(jnp.float32)
    layer_out = (resid.astype(jnp.float32) + moe + branch_weight[:, None] * dense_sum).astype(
        jnp.bfloat16
    )
    return (layer_out, new_state, new_conv_state)


def rcopy(src, dst, send, recv, ep, tp):
    return pltpu.make_async_remote_copy(
        src_ref=src,
        dst_ref=dst,
        send_sem=send,
        recv_sem=recv,
        device_id={"ep": ep, "tp": tp},
        device_id_type=pl.DeviceIdType.MESH,
    )


def greet(peers):
    barrier = pltpu.get_barrier_semaphore()
    for ep, tp in peers:
        pl.semaphore_signal(
            barrier, inc=1, device_id={"ep": ep, "tp": tp}, device_id_type=pl.DeviceIdType.MESH
        )
    pl.semaphore_wait(barrier, len(peers))


def dot(left, right):
    return jnp.dot(left, right, preferred_element_type=F32)


def split_sum(me, tp, zs, half, psend, precv, keep, rsend, rrecv, s2, r2, s3, r3, part, between):
    z, c = me // 2, me % 2
    mate = 2 * z + 1 - c
    sends = []
    for zz in range(zs):
        psend[zz] = part(zz, 1 - c)
        cp = rcopy(psend.at[zz], precv.at[zz], s2.at[zz], r2.at[zz], mate, tp)
        cp.start()
        sends.append(cp)
    for zz in range(zs):
        keep[zz] = part(zz, c).astype(F32)
    between()
    for dz in range(1, zs):
        zz = lax.rem(z + dz, zs)
        rcopy(psend.at[zz], precv.at[zz], s2.at[zz], r2.at[zz], mate, tp).wait_recv()
        rsend[zz] = (keep[zz] + precv[zz].astype(F32)).astype(BF16)
        cp = rcopy(rsend.at[zz], rrecv.at[z], s3.at[dz], r3.at[dz], 2 * zz + c, tp)
        cp.start()
        sends.append(cp)
    rcopy(psend.at[z], precv.at[z], s2.at[z], r2.at[z], mate, tp).wait_recv()

    def finish():
        total = keep[z] + precv[z].astype(F32)
        for dz in range(1, zs):
            frm = lax.rem(z - dz + zs, zs)
            rcopy(rrecv.at[frm], rrecv.at[frm], s3.at[dz], r3.at[dz], mate, tp).wait_recv()
            total += rrecv[frm].astype(F32)
        return total

    return sends, finish


def project_kernel(
    n, tokens, gain, iw, gw, out, nsend, narr, psend, precv, keep, rsend, rrecv, s1, r1, s2, r2, s3, r3
):
    me, tp = lax.axis_index("ep"), lax.axis_index("tp")
    zs = n // 2
    q, ch = iw.shape
    greet([(lax.rem(me + d, n), tp) for d in range(1, n)])
    values = tokens[...].astype(F32)
    inverse = lax.rsqrt(jnp.mean(values * values, axis=-1, keepdims=True) + epsilon)
    normed = (values * inverse * gain[...]).astype(BF16)
    for e in range(n):
        nsend[e] = normed[:, e * q : (e + 1) * q]
    sends = []
    for d in range(1, n):
        to = lax.rem(me + d, n)
        cp = rcopy(nsend.at[to], narr.at[me], s1.at[d], r1.at[d], to, tp)
        cp.start()
        sends.append(cp)
    narr[me] = nsend[me]
    for d in range(1, n):
        frm = lax.rem(me - d + n, n)
        rcopy(narr.at[frm], narr.at[frm], s1.at[d], r1.at[d], frm, tp).wait_recv()

    def part(zz, core):
        rows = narr[2 * zz + core]
        return jnp.concatenate([dot(rows, iw[...]), dot(rows, gw[...])], axis=1).astype(psend.dtype)

    more, finish = split_sum(
        me, tp, zs, None, psend, precv, keep, rsend, rrecv, s2, r2, s3, r3, part, lambda: None
    )
    out[...] = finish().astype(BF16)
    for cp in sends + more:
        cp.wait_send()


def project(n, tokens, gain, iw, gw):
    rows, width = tokens.shape
    q, ch = iw.shape
    zs = n // 2
    vm = pl.BlockSpec(memory_space=pltpu.VMEM)
    dma = pltpu.SemaphoreType.DMA
    return pl.pallas_call(
        functools.partial(project_kernel, n),
        out_shape=jax.ShapeDtypeStruct((rows, 2 * ch), BF16),
        in_specs=[vm] * 4,
        out_specs=vm,
        scratch_shapes=[
            pltpu.VMEM((n, rows, q), BF16),
            pltpu.VMEM((n, rows, q), BF16),
            pltpu.VMEM((zs, rows, 2 * ch), BF16),
            pltpu.VMEM((zs, rows, 2 * ch), BF16),
            pltpu.VMEM((zs, rows, 2 * ch), F32),
            pltpu.VMEM((zs, rows, 2 * ch), BF16),
            pltpu.VMEM((zs, rows, 2 * ch), BF16),
            dma((n,)),
            dma((n,)),
            dma((zs,)),
            dma((zs,)),
            dma((zs,)),
            dma((zs,)),
        ],
        compiler_params=pltpu.CompilerParams(
            collective_id=0, has_side_effects=True, vmem_limit_bytes=40 * 1024 * 1024
        ),
        name="project",
    )(tokens, gain, iw, gw)


def layer_kernel(
    n, m, experts, mr, ow, tokens, gain, mask, rb, dg, du, dd, eg, eu, ed, out,
    wg, wu, wd, mall, masks, osend, orecv, full, nf, accg, accu, act,
    psend, precv, dkeep, rsend, rrecv, dact, dall,
    ysend, yrecv, keep, xsend, xrecv, zsend, zrecv, fblk, fin,
    lw, ks, kr, as_, ar, bs, br, os_, or_, zs_, zr, xs, xr, ms, mrv,
    s2, r2, s3, r3, cs, cr, es, er, ys, yr, hs, hr, gs, gr, fs, fr,
):
    me, tp = lax.axis_index("ep"), lax.axis_index("tp")
    zs = n // 2
    z, c = me // 2, me % 2
    mate = 2 * z + 1 - c
    rows, width = tokens.shape
    q = ow.shape[1]
    g = q // m
    everyone = [
        (lax.rem(me + de, n), lax.rem(tp + dt, m))
        for de in range(n)
        for dt in range(m)
        if de or dt
    ]
    loads = [
        pltpu.make_async_copy(eg, wg, lw.at[n]),
        pltpu.make_async_copy(eu, wu, lw.at[n + 1]),
    ] + [
        pltpu.make_async_copy(ed.at[:, pl.ds(i * q, q)], wd.at[i], lw.at[i]) for i in range(n)
    ]
    for cp in loads:
        cp.start()
    greet(everyone)
    sends = []

    def send(*args):
        cp = rcopy(*args)
        cp.start()
        sends.append(cp)

    def arrive(buf, sem):
        rcopy(buf, buf, sem, sem, mate, tp).wait_recv()

    def zpeer(dz):
        return lax.rem(z + dz, zs)

    def zfrom(dz):
        return lax.rem(z - dz + zs, zs)

    def tto(dt):
        return lax.rem(tp + dt, m)

    def tfrom(dt):
        return lax.rem(tp - dt + m, m)

    def gather(own, buf, s_a, r_a, s_b, r_b):
        for dz in range(1, zs):
            send(own, buf.at[me], s_a.at[dz], r_a.at[dz], 2 * zpeer(dz) + c, tp)
        send(own, buf.at[me], s_b.at[0], r_b.at[0], mate, tp)
        buf[me] = own[...]
        for dz in range(1, zs):
            slot = 2 * zfrom(dz) + c
            arrive(buf.at[slot], r_a.at[dz])
            send(buf.at[slot], buf.at[slot], s_b.at[dz], r_b.at[dz], mate, tp)

    def gathered(buf, r_b):
        for dz in range(zs):
            arrive(buf.at[2 * zfrom(dz) + 1 - c], r_b.at[dz])

    gather(mr, mall, as_, ar, bs, br)
    gathered(mall, br)
    mixed = dot(mall[...].reshape(n * rows, mr.shape[1]), ow[...]).astype(BF16)
    for r in range(n):
        for t in range(m):
            osend[r, t] = mixed[r * rows : (r + 1) * rows, t * g : (t + 1) * g]
    for de in range(n):
        for dt in range(m):
            if de or dt:
                r, t = lax.rem(me + de, n), tto(dt)
                k = de * m + dt
                send(osend.at[r, t], orecv.at[tp, me], os_.at[k], or_.at[k], r, t)
    orecv[tp, me] = osend[me, tp]
    for d in range(1, n):
        to = lax.rem(me + d, n)
        send(mask, masks.at[me], ks.at[d], kr.at[d], to, tp)
    masks[me] = mask[...]
    for de in range(n):
        for dt in range(m):
            if de or dt:
                k = de * m + dt
                arrive(orecv.at[tfrom(dt), lax.rem(me - de + n, n)], or_.at[k])
    for e in range(n):
        total = orecv[0, e].astype(F32)
        for t in range(1, m):
            total += orecv[t, e].astype(F32)
        own = tokens[:, pl.ds(pl.multiple_of(e * q + tp * g, LANES), g)].astype(F32)
        full[tp, me, e] = (own + total).astype(BF16)

    def spread(slot, dz):
        for dt in range(1, m):
            k = dz * m + dt
            send(full.at[tp, slot], full.at[tp, slot], xs.at[k], xr.at[k], 2 * z + c, tto(dt))
        k = dz * m
        send(full.at[tp, slot], full.at[tp, slot], ms.at[k], mrv.at[k], mate, tp)

    for dz in range(1, zs):
        send(full.at[tp, me], full.at[tp, me], zs_.at[dz], zr.at[dz], 2 * zpeer(dz) + c, tp)
    spread(me, 0)
    for dz in range(1, zs):
        slot = 2 * zfrom(dz) + c
        arrive(full.at[tp, slot], zr.at[dz])
        spread(slot, dz)
    for dz in range(zs):
        slot = 2 * zfrom(dz) + c
        for dt in range(1, m):
            k = dz * m + dt
            arrive(full.at[tfrom(dt), slot], xr.at[k])
            send(
                full.at[tfrom(dt), slot], full.at[tfrom(dt), slot], ms.at[k], mrv.at[k], mate, tp
            )
    for dz in range(zs):
        slot = 2 * zfrom(dz) + 1 - c
        for dt in range(m):
            arrive(full.at[tfrom(dt), slot], mrv.at[dz * m + dt])

    @pl.loop(0, n)
    def _(r):
        square = jnp.zeros((rows, g), F32)
        for t in range(m):
            for e in range(n):
                v = full[t, r, e].astype(F32)
                square += v * v
        inverse = lax.rsqrt(jnp.sum(square, axis=-1, keepdims=True) / width + epsilon)
        for t in range(m):
            for e in range(n):
                at = e * q + t * g
                nf[e, r, :, t * g : (t + 1) * g] = (
                    full[t, r, e].astype(F32) * inverse * gain[:, at : at + g]
                ).astype(BF16)

    def expert_in(first, last):
        @pl.loop(first, last)
        def _(k):
            x = nf[k].reshape(n * rows, q)
            accg[...] += dot(x, wg[k])
            accu[...] += dot(x, wu[k])

    def dpart(zz, core):
        x = nf[me, 2 * zz + core]
        return jnp.concatenate([dot(x, dg[...]), dot(x, du[...])], axis=1).astype(BF16)

    def between():
        accg[...] = jnp.zeros_like(accg)
        accu[...] = jnp.zeros_like(accu)
        loads[0].wait()
        loads[1].wait()
        expert_in(0, n // 4)

    more, finish = split_sum(
        me, tp, zs, None, psend, precv, dkeep, rsend, rrecv, s2, r2, s3, r3, dpart, between
    )
    sends += more
    expert_in(n // 4, n)
    gate = accg[...]
    act[...] = (gate * jax.nn.sigmoid(gate) * accu[...]).astype(BF16)
    h = dg.shape[1]
    both = finish()
    first = both[:, :h]
    dact[...] = (first * jax.nn.sigmoid(first) * both[:, h:]).astype(BF16)
    for dz in range(1, zs):
        send(dact, dall.at[me], cs.at[dz], cr.at[dz], 2 * zpeer(dz) + c, tp)
    send(dact, dall.at[me], es.at[0], er.at[0], mate, tp)
    dall[me] = dact[...]

    logits = dot(nf[0].reshape(n * rows, q), rb[0])
    for k in range(1, n):
        logits += dot(nf[k].reshape(n * rows, q), rb[k])
    for d in range(1, n):
        arrive(masks.at[lax.rem(me - d + n, n)], kr.at[d])
    chosen = masks[...].reshape(n * rows, LANES).astype(F32)
    named = logits * chosen
    other = jnp.sum(named, axis=-1, keepdims=True) - named
    weight = (jax.nn.sigmoid(logits - other) * chosen).astype(BF16).astype(F32)
    lane = lax.broadcasted_iota(jnp.int32, (n * rows, LANES), 1)
    weight = jnp.sum(jnp.where(lane == me, weight, 0.0), axis=-1, keepdims=True)
    branch = jnp.sum(
        jnp.where(lane == experts, jax.nn.sigmoid(logits), 0.0), axis=-1, keepdims=True
    )

    for cp in loads[2:]:
        cp.wait()
    order = [lax.rem(z + 1 + i, m) for i in range(m)]
    for i in range(m):
        y = dot(act[...], wd[2 * order[i] + 1 - c]) * weight
        ysend[i] = y.astype(BF16)
        send(ysend.at[i], yrecv.at[i], ys.at[i], yr.at[i], mate, tp)
    for i in range(m):
        keep[i] = dot(act[...], wd[2 * order[i] + c]) * weight
    for dz in range(1, zs):
        slot = 2 * zfrom(dz) + c
        arrive(dall.at[slot], cr.at[dz])
        send(dall.at[slot], dall.at[slot], es.at[dz], er.at[dz], mate, tp)

    def forward(i):
        arrive(yrecv.at[i], yr.at[i])
        keep[i] = keep[i] + yrecv[i].astype(F32)

        @pl.when(order[i] != tp)
        def _():
            dt = lax.rem(order[i] - tp + m, m)
            xsend[i] = keep[i].astype(BF16)
            rcopy(
                xsend.at[i], xrecv.at[dt], hs.at[dt], hr.at[dt], me, order[i]
            ).start()

    for i in range(m - 1):
        forward(i)
    for dz in range(zs):
        arrive(dall.at[2 * zfrom(dz) + 1 - c], er.at[dz])
    keep[m - 1] = keep[m - 1] + dot(dall[...].reshape(n * rows, h), dd[...]) * branch
    forward(m - 1)

    mine = lax.rem(tp - z - 1 + 2 * m, m)
    total = keep[mine]
    for dt in range(1, m):
        arrive(xrecv.at[dt], hr.at[dt])
        total += xrecv[dt].astype(F32)
    keep[mine] = total
    for zz in range(zs):
        zsend[zz] = total[2 * zz * rows : 2 * (zz + 1) * rows].astype(BF16)
    for dz in range(1, zs):
        send(zsend.at[zpeer(dz)], zrecv.at[z], gs.at[dz], gr.at[dz], 2 * zpeer(dz) + c, tp)
    at = pl.multiple_of(2 * z * rows, rows)
    total = keep[mine, pl.ds(at, 2 * rows), :]
    for dz in range(1, zs):
        arrive(zrecv.at[zfrom(dz)], gr.at[dz])
        total += zrecv[zfrom(dz)].astype(F32)
    chunk = 2 * tp + c
    for core in range(2):
        resid = jnp.concatenate([full[t, 2 * z + core, chunk] for t in range(m)], axis=1)
        fblk[core] = (resid.astype(F32) + total[core * rows : (core + 1) * rows]).astype(BF16)
    for dc in range(2):
        for dt in range(m):
            if dc or dt:
                core = lax.rem(c + dc, 2)
                k = dc * m + dt
                send(fblk.at[core], fin.at[chunk], fs.at[k], fr.at[k], 2 * z + core, tto(dt))
    fin[chunk] = fblk[c]
    for dc in range(2):
        for dt in range(m):
            if dc or dt:
                k = dc * m + dt
                arrive(fin.at[2 * tfrom(dt) + lax.rem(c + dc, 2)], fr.at[k])
    for e in range(n):
        out[:, e * q : (e + 1) * q] = fin[e]
    for cp in sends:
        cp.wait_send()
    for dt in range(1, m):
        rcopy(xrecv.at[dt], xrecv.at[dt], hs.at[dt], hr.at[dt], mate, tp).wait_send()


def rest(n, m, experts, mr, ow, tokens, gain, mask, rb, dg, du, dd, eg, eu, ed):
    rows, width = tokens.shape
    ch, q = ow.shape
    h, f = dg.shape[1], ed.shape[0]
    g, zs, b = q // m, n // 2, n * rows
    vm = pl.BlockSpec(memory_space=pltpu.VMEM)
    hbm = pl.BlockSpec(memory_space=pl.ANY)
    v = pltpu.VMEM

    def pairs(*counts):
        return [pltpu.SemaphoreType.DMA((k,)) for k in counts for _ in range(2)]

    return pl.pallas_call(
        functools.partial(layer_kernel, n, m, experts),
        out_shape=jax.ShapeDtypeStruct((rows, width), BF16),
        in_specs=[vm] * 9 + [hbm] * 3,
        out_specs=vm,
        scratch_shapes=[
            v((n, q, f), BF16), v((n, q, f), BF16), v((n, f, q), BF16),
            v((n, rows, ch), BF16), v((n, rows, LANES), BF16),
            v((n, m, rows, g), BF16), v((m, n, rows, g), BF16),
            v((m, n, n, rows, g), BF16), v((n, n, rows, q), BF16),
            v((b, f), F32), v((b, f), F32), v((b, f), BF16),
            v((zs, rows, 2 * h), BF16), v((zs, rows, 2 * h), BF16), v((zs, rows, 2 * h), F32),
            v((zs, rows, 2 * h), BF16), v((zs, rows, 2 * h), BF16),
            v((rows, h), BF16), v((n, rows, h), BF16),
            v((m, b, q), BF16), v((m, b, q), BF16), v((m, b, q), F32),
            v((m, b, q), BF16), v((m, b, q), BF16),
            v((zs, 2 * rows, q), BF16), v((zs, 2 * rows, q), BF16),
            v((2, rows, q), BF16), v((n, rows, q), BF16),
            pltpu.SemaphoreType.DMA((n + 2,)),
        ] + pairs(n, zs, zs, n * m, zs, zs * m, zs * m, zs, zs, zs, zs, m, m, zs, 2 * m),
        compiler_params=pltpu.CompilerParams(
            collective_id=1, has_side_effects=True, vmem_limit_bytes=58 * 1024 * 1024
        ),
        name="rest",
    )(mr, ow, tokens, gain, mask, rb, dg, du, dd, eg, eu, ed)


def in_kernels(
    n, m, tokens, recur_state, conv_state, mix_gain, in_weight, gate_weight, conv_taps,
    recur_gate_blocks, input_gate_blocks, decay_rate, out_weight, ffn_gain, router_weight, routes,
    expert_gate, expert_up, expert_down, dense_gate, dense_up, dense_down, branch_gate,
):
    batch_rows, width = tokens.shape
    channels = in_weight.shape[1]
    experts = router_weight.shape[1]
    q = width // n
    lanes = lax.broadcasted_iota(jnp.int32, (batch_rows, LANES), 1)
    mask = ((routes[:, 0:1] == lanes) | (routes[:, 1:2] == lanes)).astype(BF16)
    maps = jnp.concatenate(
        [
            router_weight,
            branch_gate[:, None],
            jnp.zeros((width, LANES - experts - 1), BF16),
        ],
        axis=1,
    ).reshape(n, q, LANES)
    summed = project(n, tokens, mix_gain[None, :], in_weight, gate_weight)
    x_branch, gate_branch = summed[:, :channels], summed[:, channels:]
    window = jnp.concatenate([conv_state, x_branch[:, None, :]], axis=1)
    conv_out = jnp.sum(window.astype(F32) * conv_taps[None], axis=1).astype(BF16)
    new_conv_state = window[:, 1:, :]
    blocks = conv_out.reshape(batch_rows, recur_gate_blocks.shape[0], recur_gate_blocks.shape[1])

    def gate_of(maps_of):
        return jax.nn.sigmoid(
            jnp.einsum("bhi,hij->bhj", blocks, maps_of, preferred_element_type=F32).reshape(
                batch_rows, channels
            )
        )

    recur_gate = gate_of(recur_gate_blocks)
    input_gate = gate_of(input_gate_blocks)
    log_decay = -decay_scale * recur_gate * decay_rate
    new_state = jnp.exp(log_decay) * recur_state + jnp.sqrt(
        -jnp.expm1(2.0 * log_decay)
    ) * input_gate * conv_out.astype(F32)
    mixer_rows = (new_state * jax.nn.gelu(gate_branch.astype(F32))).astype(BF16)
    f = expert_down.shape[1]
    layer_out = rest(
        n, m, experts, mixer_rows, out_weight, tokens, ffn_gain[None, :], mask, maps,
        dense_gate, dense_up, dense_down,
        expert_gate.reshape(n, q, f), expert_up.reshape(n, q, f), expert_down[0],
    )
    return (layer_out, new_state, new_conv_state)


def solution(mesh):
    in_specs = (
        P("ep", None),
        P("ep", "tp"),
        P("ep", None, "tp"),
        P(),
        P("ep", "tp"),
        P("ep", "tp"),
        P(None, "tp"),
        P("tp", None, None),
        P("tp", None, None),
        P("tp"),
        P("tp", "ep"),
        P(),
        P(),
        P("ep", None),
        P("ep", None, "tp"),
        P("ep", None, "tp"),
        P("ep", "tp", None),
        P("ep", "tp"),
        P("ep", "tp"),
        P("tp", "ep"),
        P(),
    )
    out_specs = (P("ep", None), P("ep", "tp"), P("ep", None, "tp"))
    n, m = mesh.shape["ep"], mesh.shape["tp"]

    def body(*args):
        tokens, router, dense = args[0], args[12], args[17]
        q = tokens.shape[1] // n
        fits = n == 2 * m and n == router.shape[1] < LANES and q % (m * LANES) == 0
        fits = fits and tokens.shape[0] % 16 == 0 and dense.shape[1] % LANES == 0
        if fits:
            return in_kernels(n, m, *args)
        return on_device(*args)

    return jax.shard_map(
        body, mesh=mesh, in_specs=in_specs, out_specs=out_specs, check_vma=False
    )
```

```python
import functools

import jax
import jax.numpy as jnp
from jax import lax
from jax.experimental import pallas as pl
from jax.experimental.pallas import tpu as pltpu
from jax.sharding import PartitionSpec as P

TOP_K = 2
LANES = 128
F32 = jnp.float32
BF16 = jnp.bfloat16


epsilon = 1e-06
decay_scale = 8.0


def rms_scale(rows, gain):
    values = rows.astype(jnp.float32)
    inverse = lax.rsqrt(jnp.mean(values * values, axis=-1, keepdims=True) + epsilon)
    return (values * inverse * gain).astype(jnp.bfloat16)


def on_device(
    tokens,
    recur_state,
    conv_state,
    mix_gain,
    in_weight,
    gate_weight,
    conv_taps,
    recur_gate_blocks,
    input_gate_blocks,
    decay_rate,
    out_weight,
    ffn_gain,
    router_weight,
    routes,
    expert_gate,
    expert_up,
    expert_down,
    dense_gate,
    dense_up,
    dense_down,
    branch_gate,
):
    batch_rows, width = tokens.shape
    channels = in_weight.shape[1]
    normed = rms_scale(tokens, mix_gain)
    arrived = lax.all_to_all(normed, "ep", split_axis=1, concat_axis=0, tiled=True)
    joined = jnp.concatenate([in_weight, gate_weight], axis=1)
    summed = lax.psum_scatter(
        jnp.dot(arrived, joined, preferred_element_type=jnp.float32).astype(jnp.bfloat16),
        "ep",
        scatter_dimension=0,
        tiled=True,
    ).astype(jnp.float32)
    x_sum, gate_sum = (summed[:, :channels], summed[:, channels:])
    x_branch = x_sum.astype(jnp.bfloat16)
    gate_branch = gate_sum.astype(jnp.bfloat16)
    window = jnp.concatenate([conv_state, x_branch[:, None, :]], axis=1)
    conv_out = jnp.sum(window.astype(jnp.float32) * conv_taps[None], axis=1).astype(jnp.bfloat16)
    new_conv_state = window[:, 1:, :]
    blocks = conv_out.reshape(batch_rows, recur_gate_blocks.shape[0], recur_gate_blocks.shape[1])
    recur_gate = jax.nn.sigmoid(
        jnp.einsum(
            "bhi,hij->bhj", blocks, recur_gate_blocks, preferred_element_type=jnp.float32
        ).reshape(batch_rows, channels)
    )
    input_gate = jax.nn.sigmoid(
        jnp.einsum(
            "bhi,hij->bhj", blocks, input_gate_blocks, preferred_element_type=jnp.float32
        ).reshape(batch_rows, channels)
    )
    log_decay = -decay_scale * recur_gate * decay_rate
    new_state = jnp.exp(log_decay) * recur_state + jnp.sqrt(
        -jnp.expm1(2.0 * log_decay)
    ) * input_gate * conv_out.astype(jnp.float32)
    mixer_rows = (new_state * jax.nn.gelu(gate_branch.astype(jnp.float32))).astype(jnp.bfloat16)
    mixer_part = jnp.dot(
        mixer_rows,
        lax.all_gather(out_weight, "ep", axis=1, tiled=True),
        preferred_element_type=jnp.float32,
    )
    resid = (
        tokens.astype(jnp.float32)
        + lax.psum(mixer_part.astype(jnp.bfloat16), "tp").astype(jnp.float32)
    ).astype(jnp.bfloat16)
    normed_ffn = rms_scale(resid, ffn_gain)
    router_logits = jnp.dot(normed_ffn, router_weight, preferred_element_type=jnp.float32)
    experts = router_logits.shape[1]
    expert_ids = lax.broadcasted_iota(jnp.int32, (batch_rows, TOP_K, experts), 2)
    picked = jnp.sum(
        jnp.where(routes[:, :, None] == expert_ids, router_logits[:, None, :], 0.0), axis=2
    )
    route_weight = jax.nn.sigmoid(picked - picked[:, ::-1]).astype(jnp.bfloat16)
    capacity = 2 * batch_rows * TOP_K // experts
    flat_ids = routes.reshape(batch_rows * TOP_K)
    onehot = (
        flat_ids[:, None] == lax.broadcasted_iota(jnp.int32, (batch_rows * TOP_K, experts), 1)
    ).astype(jnp.int32)
    rank = jnp.sum((jnp.cumsum(onehot, axis=0) - onehot) * onehot, axis=1)
    slot_of = (flat_ids * capacity + rank).reshape(batch_rows, TOP_K)
    slot_rows = lax.broadcasted_iota(jnp.int32, (experts * capacity, batch_rows), 0)
    slot_cols = lax.broadcasted_iota(jnp.int32, (batch_rows, experts * capacity), 1)
    dispatch = jnp.zeros((experts * capacity, batch_rows), jnp.bfloat16)
    combine = jnp.zeros((batch_rows, experts * capacity), jnp.bfloat16)
    for pick in range(TOP_K):
        dispatch = dispatch + (slot_rows == slot_of[None, :, pick]).astype(jnp.bfloat16)
        combine = combine + jnp.where(
            slot_cols == slot_of[:, pick : pick + 1],
            route_weight[:, pick : pick + 1],
            jnp.zeros((), jnp.bfloat16),
        )
    outgoing = (
        jnp.dot(dispatch, normed_ffn, preferred_element_type=jnp.float32)
        .astype(jnp.bfloat16)
        .reshape(experts, capacity, width)
    )
    gate_local = expert_gate[0]
    up_local = expert_up[0]
    down_local = expert_down[0]
    arrived_rows = lax.all_to_all(outgoing, "ep", split_axis=0, concat_axis=0, tiled=True)
    sources, items, features = arrived_rows.shape
    rows = arrived_rows.reshape(sources * items, features)
    first = jnp.dot(rows, gate_local, preferred_element_type=jnp.float32)
    second = jnp.dot(rows, up_local, preferred_element_type=jnp.float32)
    act = (jax.nn.silu(first) * second).astype(jnp.bfloat16)
    partial_value = jnp.dot(act, down_local, preferred_element_type=jnp.float32)
    total = lax.psum(partial_value.astype(jnp.bfloat16), "tp")
    returned = lax.all_to_all(
        total.reshape(sources, items, total.shape[1]), "ep", split_axis=0, concat_axis=0, tiled=True
    )
    moe = jnp.dot(
        combine,
        returned.reshape(experts * capacity, returned.shape[2]),
        preferred_element_type=jnp.float32,
    )
    dense_arrived = lax.all_to_all(normed_ffn, "ep", split_axis=1, concat_axis=0, tiled=True)
    dense_joined = jnp.concatenate([dense_gate, dense_up], axis=1)
    dense_summed = lax.psum_scatter(
        jnp.dot(dense_arrived, dense_joined, preferred_element_type=jnp.float32).astype(
            jnp.bfloat16
        ),
        "ep",
        scatter_dimension=0,
        tiled=True,
    ).astype(jnp.float32)
    dense_first = dense_summed[:, : dense_gate.shape[1]]
    dense_second = dense_summed[:, dense_gate.shape[1] :]
    dense_act = (jax.nn.silu(dense_first) * dense_second).astype(jnp.bfloat16)
    dense_part = jnp.dot(
        dense_act,
        lax.all_gather(dense_down, "ep", axis=1, tiled=True),
        preferred_element_type=jnp.float32,
    )
    branch_weight = jax.nn.sigmoid(
        jnp.dot(normed_ffn, branch_gate, preferred_element_type=jnp.float32)
    )
    dense_sum = lax.psum(dense_part.astype(jnp.bfloat16), "tp").astype(jnp.float32)
    layer_out = (resid.astype(jnp.float32) + moe + branch_weight[:, None] * dense_sum).astype(
        jnp.bfloat16
    )
    return (layer_out, new_state, new_conv_state)


def rcopy(src, dst, send, recv, ep, tp):
    return pltpu.make_async_remote_copy(
        src_ref=src,
        dst_ref=dst,
        send_sem=send,
        recv_sem=recv,
        device_id={"ep": ep, "tp": tp},
        device_id_type=pl.DeviceIdType.MESH,
    )


def greet(peers):
    barrier = pltpu.get_barrier_semaphore()
    for ep, tp in peers:
        pl.semaphore_signal(
            barrier, inc=1, device_id={"ep": ep, "tp": tp}, device_id_type=pl.DeviceIdType.MESH
        )
    pl.semaphore_wait(barrier, len(peers))


def dot(left, right):
    return jnp.dot(left, right, preferred_element_type=F32)


def split_sum(me, tp, zs, half, psend, precv, keep, rsend, rrecv, s2, r2, s3, r3, part, between):
    z, c = me // 2, me % 2
    mate = 2 * z + 1 - c
    sends = []
    for zz in range(zs):
        psend[zz] = part(zz, 1 - c)
        cp = rcopy(psend.at[zz], precv.at[zz], s2.at[zz], r2.at[zz], mate, tp)
        cp.start()
        sends.append(cp)
    for zz in range(zs):
        keep[zz] = part(zz, c).astype(F32)
    between()
    for dz in range(1, zs):
        zz = lax.rem(z + dz, zs)
        rcopy(psend.at[zz], precv.at[zz], s2.at[zz], r2.at[zz], mate, tp).wait_recv()
        rsend[zz] = (keep[zz] + precv[zz].astype(F32)).astype(BF16)
        cp = rcopy(rsend.at[zz], rrecv.at[z], s3.at[dz], r3.at[dz], 2 * zz + c, tp)
        cp.start()
        sends.append(cp)
    rcopy(psend.at[z], precv.at[z], s2.at[z], r2.at[z], mate, tp).wait_recv()

    def finish():
        total = keep[z] + precv[z].astype(F32)
        for dz in range(1, zs):
            frm = lax.rem(z - dz + zs, zs)
            rcopy(rrecv.at[frm], rrecv.at[frm], s3.at[dz], r3.at[dz], mate, tp).wait_recv()
            total += rrecv[frm].astype(F32)
        return total

    return sends, finish


def project_kernel(
    n, tokens, gain, iw_hbm, gw_hbm, out, toks, iw, gw, lw, narr, psend, precv, keep, rsend, rrecv, s1, r1, s2, r2, s3, r3
):
    me, tp = lax.axis_index("ep"), lax.axis_index("tp")
    zs = n // 2
    q, ch = iw.shape
    g = toks.shape[2]
    loads = [
        pltpu.make_async_copy(iw_hbm, iw, lw.at[0]),
        pltpu.make_async_copy(gw_hbm, gw, lw.at[1]),
    ]
    for cp in loads:
        cp.start()
    greet([(lax.rem(me + d, n), tp) for d in range(1, n)])

    def columns(e):
        return pl.ds(pl.multiple_of(e * q, LANES), q)

    sends = []
    for d in range(1, n):
        to = lax.rem(me + d, n)
        cp = rcopy(tokens.at[:, columns(to)], narr.at[me], s1.at[d], r1.at[d], to, tp)
        cp.start()
        sends.append(cp)
    narr[me] = tokens[:, columns(me)]
    values = tokens[...].astype(F32)
    inverse = lax.rsqrt(jnp.mean(values * values, axis=-1, keepdims=True) + epsilon)
    for cp in loads:
        cp.wait()
    for d in range(1, n):
        frm = lax.rem(me - d + n, n)
        rcopy(narr.at[frm], narr.at[frm], s1.at[d], r1.at[d], frm, tp).wait_recv()

    def part(zz, core):
        rows = (narr[2 * zz + core].astype(F32) * gain[me]).astype(BF16)
        return jnp.concatenate([dot(rows, iw[...]), dot(rows, gw[...])], axis=1).astype(psend.dtype)

    more, finish = split_sum(
        me, tp, zs, None, psend, precv, keep, rsend, rrecv, s2, r2, s3, r3, part, lambda: None
    )
    toks[...] = narr[:, :, pl.ds(pl.multiple_of(tp * g, LANES), g)]
    out[...] = (finish() * inverse).astype(BF16)
    for cp in sends + more:
        cp.wait_send()


def project(n, m, tokens, gain, iw, gw):
    rows, width = tokens.shape
    q, ch = iw.shape
    zs = n // 2
    vm = pl.BlockSpec(memory_space=pltpu.VMEM)
    dma = pltpu.SemaphoreType.DMA
    return pl.pallas_call(
        functools.partial(project_kernel, n),
        out_shape=(
            jax.ShapeDtypeStruct((rows, 2 * ch), BF16),
            jax.ShapeDtypeStruct((n, rows, q // m), BF16),
        ),
        in_specs=[vm] * 2 + [pl.BlockSpec(memory_space=pl.ANY)] * 2,
        out_specs=(vm, vm),
        scratch_shapes=[
            pltpu.VMEM((q, ch), BF16),
            pltpu.VMEM((q, ch), BF16),
            dma((2,)),
            pltpu.VMEM((n, rows, q), BF16),
            pltpu.VMEM((zs, rows, 2 * ch), BF16),
            pltpu.VMEM((zs, rows, 2 * ch), BF16),
            pltpu.VMEM((zs, rows, 2 * ch), F32),
            pltpu.VMEM((zs, rows, 2 * ch), BF16),
            pltpu.VMEM((zs, rows, 2 * ch), BF16),
            dma((n,)),
            dma((n,)),
            dma((zs,)),
            dma((zs,)),
            dma((zs,)),
            dma((zs,)),
        ],
        compiler_params=pltpu.CompilerParams(
            collective_id=0, has_side_effects=True, vmem_limit_bytes=60 * 1024 * 1024
        ),
        name="project",
    )(tokens, gain, iw, gw)


def layer_kernel(
    n, m, experts, mr, toks, gain, mask, rb, bg, ow_hbm, dg_hbm, du_hbm, dd_hbm, eg, eu, ed, out,
    ow, dg, du, dd, lacc, square, bacc, wg, wu, wd, mall, masks, osend, orecv, full, nf, accg, accu, act,
    psend, precv, dkeep, rsend, rrecv, dact, dall,
    ysend, yrecv, keep, xsend, xrecv, zsend, zrecv, fblk, fin,
    lw, ks, kr, as_, ar, bs, br, os_, or_, zs_, zr, xs, xr, ms, mrv,
    s2, r2, s3, r3, cs, cr, es, er, ys, yr, hs, hr, gs, gr, fs, fr,
):
    me, tp = lax.axis_index("ep"), lax.axis_index("tp")
    zs = n // 2
    z, c = me // 2, me % 2
    mate = 2 * z + 1 - c
    rows, width = out.shape
    q = ow.shape[1]
    g = q // m
    peers = [(lax.rem(me + d, n), tp) for d in range(1, n)]
    for d in range(1, m):
        peers += [(me, lax.rem(tp + d, m)), (mate, lax.rem(tp + d, m))]
    small = [
        pltpu.make_async_copy(a, b, lw.at[n + 2 + k])
        for k, (a, b) in enumerate(((ow_hbm, ow), (dg_hbm, dg), (du_hbm, du), (dd_hbm, dd)))
    ]
    for cp in small:
        cp.start()
    loads = [
        pltpu.make_async_copy(eg, wg, lw.at[n]),
        pltpu.make_async_copy(eu, wu, lw.at[n + 1]),
    ] + [
        pltpu.make_async_copy(ed.at[:, pl.ds(i * q, q)], wd.at[i], lw.at[i]) for i in range(n)
    ]
    for cp in loads:
        cp.start()
    greet(peers)
    sends = []

    def send(*args):
        cp = rcopy(*args)
        cp.start()
        sends.append(cp)

    def arrive(buf, sem):
        rcopy(buf, buf, sem, sem, mate, tp).wait_recv()

    def zpeer(dz):
        return lax.rem(z + dz, zs)

    def zfrom(dz):
        return lax.rem(z - dz + zs, zs)

    def tto(dt):
        return lax.rem(tp + dt, m)

    def tfrom(dt):
        return lax.rem(tp - dt + m, m)

    def gather(own, buf, s_a, r_a, s_b, r_b):
        for dz in range(1, zs):
            send(own, buf.at[me], s_a.at[dz], r_a.at[dz], 2 * zpeer(dz) + c, tp)
        send(own, buf.at[me], s_b.at[0], r_b.at[0], mate, tp)
        buf[me] = own[...]
        for dz in range(1, zs):
            slot = 2 * zfrom(dz) + c
            arrive(buf.at[slot], r_a.at[dz])
            send(buf.at[slot], buf.at[slot], s_b.at[dz], r_b.at[dz], mate, tp)

    def gathered(buf, r_b):
        for dz in range(zs):
            arrive(buf.at[2 * zfrom(dz) + 1 - c], r_b.at[dz])

    gather(mr, mall, as_, ar, bs, br)
    for d in range(1, n):
        send(mask, masks.at[me], ks.at[d], kr.at[d], lax.rem(me + d, n), tp)
    masks[me] = mask[...]
    for cp in small:
        cp.wait()
    gathered(mall, br)
    mixed = dot(mall[...].reshape(n * rows, mr.shape[1]), ow[...]).astype(BF16)
    for t in range(m):
        osend[t] = mixed[:, t * g : (t + 1) * g].reshape(n, rows, g)
    for dt in range(1, m):
        send(osend.at[tto(dt)], orecv.at[tp], os_.at[dt], or_.at[dt], me, tto(dt))
    total = toks[...].astype(F32) + osend[tp].astype(F32)
    accg[...] = jnp.zeros_like(accg)
    accu[...] = jnp.zeros_like(accu)
    lacc[...] = jnp.zeros_like(lacc)
    square[...] = jnp.zeros_like(square)
    bacc[...] = jnp.zeros_like(bacc)
    for dt in range(1, m):
        arrive(orecv.at[tfrom(dt)], or_.at[dt])
        total += orecv[tfrom(dt)].astype(F32)
    full[tp, me] = total.astype(BF16)

    def spread(slot, dz):
        for dt in range(1, m):
            k = dz * m + dt
            send(full.at[tp, slot], full.at[tp, slot], xs.at[k], xr.at[k], 2 * z + c, tto(dt))
        k = dz * m
        send(full.at[tp, slot], full.at[tp, slot], ms.at[k], mrv.at[k], mate, tp)

    for dz in range(1, zs):
        send(full.at[tp, me], full.at[tp, me], zs_.at[dz], zr.at[dz], 2 * zpeer(dz) + c, tp)
    spread(me, 0)
    for dz in range(1, zs):
        slot = 2 * zfrom(dz) + c
        arrive(full.at[tp, slot], zr.at[dz])
        spread(slot, dz)
    def relay(dz):
        slot = 2 * zfrom(dz) + c
        for dt in range(1, m):
            k = dz * m + dt
            at = full.at[tfrom(dt), slot]
            arrive(at, xr.at[k])
            send(at, at, ms.at[k], mrv.at[k], mate, tp)

    def expert_in(dz):
        slot = 2 * zfrom(dz) + 1 - c
        for dt in range(m):
            arrive(full.at[tfrom(dt), slot], mrv.at[dz * m + dt])

        @pl.loop(0, 2)
        def _(core):
            e = 2 * zfrom(dz) + core
            for t in range(m):
                at = slice(t * g, (t + 1) * g)
                v = full[t, e].reshape(n * rows, g).astype(F32)
                square[...] += v * v
                scaled = (v * gain[e, :, at]).astype(BF16)
                bacc[...] += scaled.astype(F32) * bg[e, :, at].astype(F32)
                nf[e, :, :, at] = scaled.reshape(n, rows, g)
            x = nf[e].reshape(n * rows, q)
            accg[...] += dot(x, wg[e])
            accu[...] += dot(x, wu[e])
            maps = rb[:, pl.ds(pl.multiple_of(e * q, LANES), q)]
            lacc[...] += lax.dot_general(
                x, maps, (((1,), (1,)), ((), ())), preferred_element_type=F32
            )

    loads[0].wait()
    loads[1].wait()
    relay(0)
    relay(1)
    expert_in(0)

    def dpart(zz, core):
        x = nf[me, 2 * zz + core]
        return jnp.concatenate([dot(x, dg[...]), dot(x, du[...])], axis=1).astype(BF16)

    def between():
        for dz in range(2, zs):
            relay(dz)
        expert_in(1)

    more, finish = split_sum(
        me, tp, zs, None, psend, precv, dkeep, rsend, rrecv, s2, r2, s3, r3, dpart, between
    )
    sends += more
    for dz in range(2, zs):
        expert_in(dz)
    inverse = lax.rsqrt(jnp.sum(square[...], axis=-1, keepdims=True) / width + epsilon)
    gate = accg[...] * inverse
    act[...] = (gate * jax.nn.sigmoid(gate) * (accu[...] * inverse)).astype(BF16)
    h = dg.shape[1]
    square[:, 0:1] = inverse
    both = finish() * square[pl.ds(pl.multiple_of(me * rows, rows), rows), 0:1]
    first = both[:, :h]
    dact[...] = (first * jax.nn.sigmoid(first) * both[:, h:]).astype(BF16)
    for dz in range(1, zs):
        send(dact, dall.at[me], cs.at[dz], cr.at[dz], 2 * zpeer(dz) + c, tp)
    send(dact, dall.at[me], es.at[0], er.at[0], mate, tp)
    dall[me] = dact[...]

    logits = lacc[...] * inverse
    for d in range(1, n):
        arrive(masks.at[lax.rem(me - d + n, n)], kr.at[d])
    chosen = masks[...].reshape(n * rows, LANES)[:, :experts].astype(F32)
    named = logits * chosen
    other = jnp.sum(named, axis=-1, keepdims=True) - named
    weight = (jax.nn.sigmoid(logits - other) * chosen).astype(BF16).astype(F32)
    lane = lax.broadcasted_iota(jnp.int32, (n * rows, experts), 1)
    weight = jnp.sum(jnp.where(lane == me, weight, 0.0), axis=-1, keepdims=True)
    branch = jax.nn.sigmoid(jnp.sum(bacc[...], axis=-1, keepdims=True) * inverse)

    for cp in loads[2:]:
        cp.wait()
    order = [lax.rem(z + 1 + i, m) for i in range(m)]
    for i in range(m):
        y = dot(act[...], wd[2 * order[i] + 1 - c]) * weight
        ysend[i] = y.astype(BF16)
        send(ysend.at[i], yrecv.at[i], ys.at[i], yr.at[i], mate, tp)
    for i in range(m):
        keep[i] = dot(act[...], wd[2 * order[i] + c]) * weight
    for dz in range(1, zs):
        slot = 2 * zfrom(dz) + c
        arrive(dall.at[slot], cr.at[dz])
        send(dall.at[slot], dall.at[slot], es.at[dz], er.at[dz], mate, tp)

    def forward(i):
        arrive(yrecv.at[i], yr.at[i])
        keep[i] = keep[i] + yrecv[i].astype(F32)

        @pl.when(order[i] != tp)
        def _():
            dt = lax.rem(order[i] - tp + m, m)
            xsend[i] = keep[i].astype(BF16)
            rcopy(
                xsend.at[i], xrecv.at[dt], hs.at[dt], hr.at[dt], me, order[i]
            ).start()

    for i in range(m - 1):
        forward(i)
    for dz in range(zs):
        arrive(dall.at[2 * zfrom(dz) + 1 - c], er.at[dz])
    keep[m - 1] = keep[m - 1] + dot(dall[...].reshape(n * rows, h), dd[...]) * branch
    forward(m - 1)

    mine = lax.rem(tp - z - 1 + 2 * m, m)
    total = keep[mine]
    for dt in range(1, m):
        arrive(xrecv.at[dt], hr.at[dt])
        total += xrecv[dt].astype(F32)
    keep[mine] = total
    for zz in range(zs):
        zsend[zz] = total[2 * zz * rows : 2 * (zz + 1) * rows].astype(BF16)
    for dz in range(1, zs):
        send(zsend.at[zpeer(dz)], zrecv.at[z], gs.at[dz], gr.at[dz], 2 * zpeer(dz) + c, tp)
    at = pl.multiple_of(2 * z * rows, rows)
    total = keep[mine, pl.ds(at, 2 * rows), :]
    for dz in range(1, zs):
        arrive(zrecv.at[zfrom(dz)], gr.at[dz])
        total += zrecv[zfrom(dz)].astype(F32)
    chunk = 2 * tp + c
    for core in range(2):
        resid = jnp.concatenate([full[t, chunk, 2 * z + core] for t in range(m)], axis=1)
        fblk[core] = (resid.astype(F32) + total[core * rows : (core + 1) * rows]).astype(BF16)
    for dc in range(2):
        for dt in range(m):
            if dc or dt:
                core = lax.rem(c + dc, 2)
                k = dc * m + dt
                send(fblk.at[core], fin.at[chunk], fs.at[k], fr.at[k], 2 * z + core, tto(dt))
    fin[chunk] = fblk[c]
    for dc in range(2):
        for dt in range(m):
            if dc or dt:
                k = dc * m + dt
                arrive(fin.at[2 * tfrom(dt) + lax.rem(c + dc, 2)], fr.at[k])
    for e in range(n):
        out[:, e * q : (e + 1) * q] = fin[e]
    for cp in sends:
        cp.wait_send()
    for dt in range(1, m):
        rcopy(xrecv.at[dt], xrecv.at[dt], hs.at[dt], hr.at[dt], mate, tp).wait_send()


def rest(n, m, experts, mr, toks, gain, mask, rb, bg, ow, dg, du, dd, eg, eu, ed):
    rows, width = mr.shape[0], ow.shape[1] * n
    ch, q = ow.shape
    h, f = dg.shape[1], ed.shape[0]
    g, zs, b = q // m, n // 2, n * rows
    vm = pl.BlockSpec(memory_space=pltpu.VMEM)
    hbm = pl.BlockSpec(memory_space=pl.ANY)
    v = pltpu.VMEM

    def pairs(*counts):
        return [pltpu.SemaphoreType.DMA((k,)) for k in counts for _ in range(2)]

    return pl.pallas_call(
        functools.partial(layer_kernel, n, m, experts),
        out_shape=jax.ShapeDtypeStruct((rows, width), BF16),
        in_specs=[vm] * 6 + [hbm] * 7,
        out_specs=vm,
        scratch_shapes=[
            v((ch, q), BF16), v((q, h), BF16), v((q, h), BF16), v((h, q), BF16),
            v((b, experts), F32), v((b, g), F32), v((b, g), F32),
            v((n, q, f), BF16), v((n, q, f), BF16), v((n, f, q), BF16),
            v((n, rows, ch), BF16), v((n, rows, LANES), BF16),
            v((m, n, rows, g), BF16), v((m, n, rows, g), BF16),
            v((m, n, n, rows, g), BF16), v((n, n, rows, q), BF16),
            v((b, f), F32), v((b, f), F32), v((b, f), BF16),
            v((zs, rows, 2 * h), BF16), v((zs, rows, 2 * h), BF16), v((zs, rows, 2 * h), F32),
            v((zs, rows, 2 * h), BF16), v((zs, rows, 2 * h), BF16),
            v((rows, h), BF16), v((n, rows, h), BF16),
            v((m, b, q), BF16), v((m, b, q), BF16), v((m, b, q), F32),
            v((m, b, q), BF16), v((m, b, q), BF16),
            v((zs, 2 * rows, q), BF16), v((zs, 2 * rows, q), BF16),
            v((2, rows, q), BF16), v((n, rows, q), BF16),
            pltpu.SemaphoreType.DMA((n + 6,)),
        ] + pairs(n, zs, zs, m, zs, zs * m, zs * m, zs, zs, zs, zs, m, m, zs, 2 * m),
        compiler_params=pltpu.CompilerParams(
            collective_id=1, has_side_effects=True, vmem_limit_bytes=58 * 1024 * 1024
        ),
        name="rest",
    )(mr, toks, gain, mask, rb, bg, ow, dg, du, dd, eg, eu, ed)


def in_kernels(
    n, m, tokens, recur_state, conv_state, mix_gain, in_weight, gate_weight, conv_taps,
    recur_gate_blocks, input_gate_blocks, decay_rate, out_weight, ffn_gain, router_weight, routes,
    expert_gate, expert_up, expert_down, dense_gate, dense_up, dense_down, branch_gate,
):
    batch_rows, width = tokens.shape
    channels = in_weight.shape[1]
    experts = router_weight.shape[1]
    q = width // n
    lanes = lax.broadcasted_iota(jnp.int32, (batch_rows, LANES), 1)
    mask = ((routes[:, 0:1] == lanes) | (routes[:, 1:2] == lanes)).astype(BF16)
    summed, toks = project(n, m, tokens, mix_gain.reshape(n, 1, q), in_weight, gate_weight)
    x_branch, gate_branch = summed[:, :channels], summed[:, channels:]
    window = jnp.concatenate([conv_state, x_branch[:, None, :]], axis=1)
    conv_out = jnp.sum(window.astype(F32) * conv_taps[None], axis=1).astype(BF16)
    new_conv_state = window[:, 1:, :]
    blocks = conv_out.reshape(batch_rows, recur_gate_blocks.shape[0], recur_gate_blocks.shape[1])

    def gate_of(maps_of):
        return jax.nn.sigmoid(
            jnp.einsum("bhi,hij->bhj", blocks, maps_of, preferred_element_type=F32).reshape(
                batch_rows, channels
            )
        )

    recur_gate = gate_of(recur_gate_blocks)
    input_gate = gate_of(input_gate_blocks)
    log_decay = -decay_scale * recur_gate * decay_rate
    new_state = jnp.exp(log_decay) * recur_state + jnp.sqrt(
        -jnp.expm1(2.0 * log_decay)
    ) * input_gate * conv_out.astype(F32)
    mixer_rows = (new_state * jax.nn.gelu(gate_branch.astype(F32))).astype(BF16)
    f = expert_down.shape[1]
    layer_out = rest(
        n, m, experts, mixer_rows, toks, ffn_gain.reshape(n, 1, q), mask,
        router_weight.T, branch_gate.reshape(n, 1, q), out_weight, dense_gate, dense_up, dense_down,
        expert_gate.reshape(n, q, f), expert_up.reshape(n, q, f), expert_down[0],
    )
    return (layer_out, new_state, new_conv_state)


def solution(mesh):
    in_specs = (
        P("ep", None),
        P("ep", "tp"),
        P("ep", None, "tp"),
        P(),
        P("ep", "tp"),
        P("ep", "tp"),
        P(None, "tp"),
        P("tp", None, None),
        P("tp", None, None),
        P("tp"),
        P("tp", "ep"),
        P(),
        P(),
        P("ep", None),
        P("ep", None, "tp"),
        P("ep", None, "tp"),
        P("ep", "tp", None),
        P("ep", "tp"),
        P("ep", "tp"),
        P("tp", "ep"),
        P(),
    )
    out_specs = (P("ep", None), P("ep", "tp"), P("ep", None, "tp"))
    n, m = mesh.shape["ep"], mesh.shape["tp"]

    def body(*args):
        tokens, router, dense = args[0], args[12], args[17]
        q = tokens.shape[1] // n
        fits = n == 2 * m and n == router.shape[1] < LANES and q % (m * LANES) == 0
        fits = fits and tokens.shape[0] % 16 == 0 and dense.shape[1] % LANES == 0
        if fits:
            return in_kernels(n, m, *args)
        return on_device(*args)

    return jax.shard_map(
        body, mesh=mesh, in_specs=in_specs, out_specs=out_specs, check_vma=False
    )
```
